32 devices in a mesh: grp: 2 (over y), dp: 2 (over x), kv: 4 (over z), tp: 2 (over core).
Axes of the slice: x: 2, y: 2, z: 4, core: 2. Of those that a mesh axis runs over, the one named last changes fastest.
Arguments:
- tokens: bfloat16 [64, 4, 4096], P(('grp', 'dp'), None, 'kv'), parts along dimension 0, may hold values from -6 to 6
- w_query: bfloat16 [4096, 2048], P('kv', 'tp'), may hold values from -0.09375 to 0.09375
- w_forget: bfloat16 [4096, 2048], P('kv', 'tp'), may hold values from -0.09375 to 0.09375
- w_input: bfloat16 [4096, 2048], P('kv', 'tp'), may hold values from -0.09375 to 0.09375
- w_gate: bfloat16 [4096, 2048], P('kv', 'tp'), may hold values from -0.09375 to 0.09375
- w_out: bfloat16 [2048, 4096], P('tp', 'kv'), may hold values from -0.125 to 0.125
- gain: float32 [4096], replicated, may hold values from 0.1 to 1.9
- head_gain: float32 [2048], replicated, may hold values from 0.1 to 1.9
- lower_bound: float32 [2048], replicated, may hold values from 0.05 to 0.9
- state: float32 [64, 16, 128, 128], P(('grp', 'dp', 'kv'), 'tp'), parts along dimension 0, may hold values from -2.4 to 2.4
- last_forget: float32 [64, 4, 2048], P(('grp', 'dp', 'kv'), None, 'tp'), parts along dimension 0, may hold values from 0.3 to 0.99
- last_values: bfloat16 [64, 4, 2048], P(('grp', 'dp', 'kv'), None, 'tp'), parts along dimension 0, may hold values from -6 to 6
- accepted: int32 [64], P(('grp', 'dp', 'kv')), parts along dimension 0, may hold values from 0 to 4
Outputs:
- mixed_out: bfloat16 [64, 4, 4096], P(('grp', 'dp'), None, ('kv', 'tp')), parts along dimension 0
- taken: float32 [64, 16, 128, 128], P(('grp', 'dp', 'kv'), 'tp'), parts along dimension 0
The draws below stay inside these ranges and needn't reach their ends.
There are 2 independent parts, one for each index of `grp`. The reference program is written for one: setup_inputs(seed, part) draws one part's arguments, and reference() takes and returns one part's arrays. A program takes and returns all parts, laid end to end along the dimension named above; an argument that names none is the same for every part. Nothing has to cross between parts.
All inputs are finite; a program needn't handle non-finite values.
Results may differ from the reference program's by a relative error of at most 0.0071.
Values may be sent and summed in bfloat16 or wider, within the bound.
No kernel may reach another device: no remote copies, remote signals or barrier semaphores. Data moves between devices by JAX's collectives and lax.ppermute only.
A program may use at most 64 MiB of HBM per device.

```python
import jax
import jax.numpy as jnp
from jax import lax

D = 4096
HEADS = 16
HEAD = 128
PROPOSALS = 4
SEQS = 32
N_TP = 2


def touch_ends(drawn, rng, least, high):
    longest = drawn.shape.index(max(drawn.shape))
    spots = []
    for shift in (0, 1):
        where = [jax.random.randint(jax.random.fold_in(rng, axis), (), 0, length) for axis, length in enumerate(drawn.shape)]
        where[longest] = (where[longest] + shift) % drawn.shape[longest]
        spots.append(tuple(where))
    return drawn.at[spots[0]].set(least).at[spots[1]].set(high)


def shard_levels(stream_key, extent, pieces, smallest, high):
    level = 1.0
    for dim, blocks in pieces:
        steps = jax.random.uniform(jax.random.fold_in(jax.random.fold_in(stream_key, 6), dim), (blocks,), jnp.float32, smallest / len(pieces), high / len(pieces))
        level = level * jnp.repeat(jnp.exp(steps), extent[dim] // blocks).reshape((-1,) + (1,) * (len(extent) - 1 - dim))
    return level


def bell_draw(key, shape, spread, most, pieces=(), held_as=jnp.bfloat16):
    array = jax.random.normal(key, shape, jnp.float32) * spread
    if len(pieces) > 0:
        array = shard_levels(key, shape, pieces, -0.22, 0.18) * array
    return jnp.clip(array, min=-most, max=most).astype(held_as)


def setup_inputs(seed: int = 0, part: int = 0) -> dict:
    keys = jax.random.split(jax.random.key(seed), 14)
    part_keys = jax.random.split(jax.random.fold_in(keys[13], part), 14)
    return {
        "tokens": bell_draw(part_keys[0], (SEQS, PROPOSALS, D), 1.0, 6.0, ((0, 2), (2, 4))),
        "w_query": bell_draw(keys[1], (D, HEADS * HEAD), D ** -0.5, 0.09375, ((0, 4), (1, 2))),
        "w_forget": bell_draw(keys[2], (D, HEADS * HEAD), D ** -0.5, 0.09375, ((0, 4), (1, 2))),
        "w_input": bell_draw(keys[3], (D, HEADS * HEAD), D ** -0.5, 0.09375, ((0, 4), (1, 2))),
        "w_gate": bell_draw(keys[4], (D, HEADS * HEAD), D ** -0.5, 0.09375, ((0, 4), (1, 2))),
        "w_out": bell_draw(keys[5], (HEADS * HEAD, D), (HEADS * HEAD) ** -0.5, 0.125, ((0, 2), (1, 4))),
        "gain": jnp.clip(1.0 + 0.18 * jax.random.normal(keys[6], (D,), jnp.float32), 0.1, 1.9),
        "head_gain": jnp.clip(1.0 + 0.18 * jax.random.normal(keys[7], (HEADS * HEAD,), jnp.float32), 0.1, 1.9),
        "lower_bound": jnp.clip(jax.random.uniform(keys[8], (HEADS * HEAD,), jnp.float32, 0.05, 0.9), 0.05, 0.9),
        "state": bell_draw(part_keys[9], (SEQS, HEADS, HEAD, HEAD), 0.3, 2.4, ((0, 8), (1, 2)), jnp.float32),
        "last_forget": jnp.clip(0.3 + 0.69 * jax.random.uniform(part_keys[10], (SEQS, PROPOSALS, HEADS * HEAD), jnp.float32) ** shard_levels(part_keys[10], (SEQS, PROPOSALS, HEADS * HEAD), ((0, 8), (2, 2)), -0.2, 0.2), 0.3, 0.99),
        "last_values": bell_draw(part_keys[11], (SEQS, PROPOSALS, HEADS * HEAD), 1.0, 6.0, ((0, 8), (2, 2))),
        "accepted": touch_ends(jax.random.randint(part_keys[12], (SEQS,), 0, PROPOSALS + 1), jax.random.fold_in(part_keys[12], 1), 0, PROPOSALS).astype(jnp.int32),
    }


EPSILON = 1e-05

def reference(tokens, w_query, w_forget, w_input, w_gate, w_out, gain, head_gain, lower_bound, state, last_forget, last_values, accepted):
    seqs, props, width = tokens.shape
    heads = w_query.shape[1] // HEAD
    tokens_f32 = tokens.astype(jnp.float32)
    row_scale = lax.rsqrt(lax.optimization_barrier(jnp.mean(tokens_f32 * tokens_f32, -1)) + EPSILON).reshape(-1, 1)
    scaled = (tokens_f32 * gain).astype(jnp.bfloat16).reshape(-1, width)

    def project(weight):
        product = jnp.dot(scaled, weight, preferred_element_type=jnp.float32) * row_scale
        return product.reshape(seqs, props, heads, HEAD)
    floor_gate = lower_bound.reshape(heads, HEAD)
    forget = floor_gate + (1.0 - floor_gate) * jax.nn.sigmoid(project(w_forget))
    queries = jax.nn.silu(project(w_query)) * HEAD ** (-0.5)
    values_new = project(w_input)
    gate_path = jax.nn.silu(project(w_gate))
    old_forget = last_forget.reshape(seqs, props, heads, HEAD)
    old_values = last_values.astype(jnp.float32).reshape(seqs, props, heads, HEAD)
    taken = state
    for position in range(PROPOSALS):
        advanced = old_forget[:, position, :, :, None] * taken + (1.0 - old_forget[:, position])[..., None] * old_values[:, position, :, None, :]
        taken = jnp.where((position < accepted)[:, None, None, None], advanced, taken)
    carried = taken
    outputs = []
    for position in range(PROPOSALS):
        carried = forget[:, position, :, :, None] * carried + (1.0 - forget[:, position])[..., None] * values_new[:, position, :, None, :]
        outputs.append(jnp.einsum('shk,shkv->shv', queries[:, position], carried, precision=lax.Precision.HIGHEST))
    recurrent = jnp.stack(outputs, 1)
    normed = recurrent * lax.rsqrt(lax.optimization_barrier(jnp.mean(recurrent * recurrent, -1, keepdims=True)) + EPSILON)
    heads_out = (normed * head_gain.reshape(heads, HEAD) * gate_path).astype(jnp.bfloat16).reshape(seqs * props, heads * HEAD)
    head_cols = heads * HEAD // N_TP
    summed = jnp.zeros((seqs * props, width), jnp.float32)
    for group in range(N_TP):
        part = jnp.dot(heads_out[:, group * head_cols:(group + 1) * head_cols], w_out[group * head_cols:(group + 1) * head_cols], preferred_element_type=jnp.float32)
        summed = summed + lax.optimization_barrier(part.astype(jnp.bfloat16)).astype(jnp.float32)
    return (summed.astype(jnp.bfloat16).reshape(seqs, props, width), taken)
```

```python
import functools

import jax
import jax.numpy as jnp
from jax import lax
from jax.experimental import pallas as pl
from jax.experimental.pallas import tpu as pltpu
from jax.sharding import PartitionSpec as P

HEAD = 128
EPSILON = 1e-05
LANES = 128


def vmem_spec():
    return pl.BlockSpec(memory_space=pltpu.VMEM)


def project_kernel(tokens, gain, wq, wf, wi, wg, *rest, ring, own_seqs, props):
    outs, (rows_ref, scaled_ref) = rest[:ring], rest[ring:]
    step = pl.program_id(0)
    place = lax.axis_index("kv")
    feat = tokens.shape[2]
    own_rows = own_seqs * props
    head_cols = outs[0].shape[1] // 4 - LANES // 4
    block = wq.shape[1]

    @pl.when(step == 0)
    def _():
        for shift in range(ring):
            source = lax.rem(place + shift, ring) * own_seqs
            for seq in range(own_seqs):
                at = shift * own_rows + seq * props
                rows_ref[at : at + props, :] = tokens[source + seq].astype(jnp.float32)
        rows = rows_ref[...]
        local_gain = gain[:, pl.ds(pl.multiple_of(place * feat, LANES), feat)]
        scaled_ref[...] = (rows * local_gain).astype(jnp.bfloat16)
        total = jnp.sum(rows * rows, axis=1, keepdims=True)
        upper = total.astype(jnp.bfloat16).astype(jnp.float32)
        lane = lax.broadcasted_iota(jnp.int32, (rows.shape[0], LANES), 1)
        packed = jnp.where(lane == 0, upper, jnp.where(lane == 1, total - upper, 0.0))
        for shift in range(ring):
            outs[shift][:, 4 * head_cols :] = packed[
                shift * own_rows : (shift + 1) * own_rows
            ].astype(jnp.bfloat16)

    for index, weight in enumerate((wq, wf, wi, wg)):
        product = jnp.dot(scaled_ref[...], weight[...], preferred_element_type=jnp.float32)
        product = product.astype(jnp.bfloat16)
        at = pl.multiple_of(index * head_cols + step * block, LANES)
        for shift in range(ring):
            outs[shift][:, pl.ds(at, block)] = product[shift * own_rows : (shift + 1) * own_rows]


def taken_kernel(accepted, state, forget, values, taken):
    count = accepted[pl.program_id(0)]
    gates = forget[0]
    props, _ = gates.shape
    heads = state.shape[1]
    fresh = values[0].astype(jnp.float32)
    tail = jnp.ones_like(gates[:1])
    weights = [None] * props
    for at in reversed(range(props)):
        live = at < count
        gate = gates[at : at + 1]
        weights[at] = jnp.where(live, (1.0 - gate) * tail, 0.0)
        tail = jnp.where(live, gate * tail, tail)
    pad = jnp.zeros((8 - (props + 1) % 8, gates.shape[1]), jnp.float32)
    stacked = jnp.concatenate([tail] + weights + [pad], axis=0)
    for head in range(heads):
        cols = slice(head * HEAD, (head + 1) * HEAD)
        turned = stacked[:, cols].T
        total = turned[:, 0:1] * state[0, head]
        for at in range(props):
            total = total + turned[:, at + 1 : at + 2] * fresh[at : at + 1, cols]
        taken[0, head] = total


def recur_kernel(*refs, ring, own_seqs, props, width):
    chunks = refs[:ring]
    floor, head_gain, taken_hbm, out, taken, sem = refs[ring:]
    copy = pltpu.make_async_copy(taken_hbm, taken, sem)
    copy.start()
    own_rows = own_seqs * props
    head_cols = out.shape[1]
    heads = head_cols // HEAD
    at_tp = pl.multiple_of(lax.axis_index("tp") * head_cols, LANES)
    floor_row = floor[:, pl.ds(at_tp, head_cols)]
    gain_row = head_gain[:, pl.ds(at_tp, head_cols)]

    def summed(start, size):
        total = chunks[0][:, start : start + size].astype(jnp.float32)
        for chunk in chunks[1:]:
            total = total + chunk[:, start : start + size].astype(jnp.float32)
        return total

    squares = jnp.sum(summed(4 * head_cols, LANES), axis=1, keepdims=True)
    row_scale = lax.rsqrt(squares / width + EPSILON)
    query_in = summed(0, head_cols) * row_scale
    queries = query_in * jax.nn.sigmoid(query_in) * HEAD ** (-0.5)
    forget = floor_row + (1.0 - floor_row) * jax.nn.sigmoid(
        summed(head_cols, head_cols) * row_scale
    )
    values = summed(2 * head_cols, head_cols) * row_scale
    gate_in = summed(3 * head_cols, head_cols) * row_scale
    gate = gate_in * jax.nn.sigmoid(gate_in) * gain_row
    keys = 1.0 - forget

    place = lax.broadcasted_iota(jnp.int32, (own_rows, 1), 0)
    token = lax.rem(place, props)
    seq = place // props
    decayed = queries
    entry = jnp.zeros_like(queries)
    recurrent = [jnp.zeros((own_rows, HEAD), jnp.float32) for _ in range(heads)]
    for back in range(props):
        old_keys = pltpu.roll(keys, back, 0) if back else keys
        old_values = pltpu.roll(values, back, 0) if back else values
        old_forget = pltpu.roll(forget, back, 0) if back else forget
        pair = decayed * old_keys
        for head in range(heads):
            cols = slice(head * HEAD, (head + 1) * HEAD)
            score = jnp.sum(pair[:, cols], axis=1, keepdims=True)
            score = jnp.where(token >= back, score, 0.0)
            recurrent[head] = recurrent[head] + score * old_values[:, cols]
        decayed = decayed * old_forget
        entry = jnp.where(token == back, decayed, entry)
    spread = []
    for head in range(heads):
        cols = slice(head * HEAD, (head + 1) * HEAD)
        spread.append(
            jnp.concatenate(
                [jnp.where(seq == one, entry[:, cols], 0.0) for one in range(own_seqs)], axis=1
            )
        )
    copy.wait()
    for head in range(heads):
        cols = slice(head * HEAD, (head + 1) * HEAD)
        start = taken[:, head].reshape(own_seqs * HEAD, HEAD)
        start_high = start.astype(jnp.bfloat16)
        start_low = (start - start_high.astype(jnp.float32)).astype(jnp.bfloat16)
        left_high = spread[head].astype(jnp.bfloat16)
        left_low = (spread[head] - left_high.astype(jnp.float32)).astype(jnp.bfloat16)
        first = jnp.dot(
            jnp.concatenate([left_high, left_low], axis=0),
            start_high,
            preferred_element_type=jnp.float32,
        )
        second = jnp.dot(left_high, start_low, preferred_element_type=jnp.float32)
        whole = recurrent[head] + first[:own_rows] + first[own_rows:] + second
        scale = lax.rsqrt(jnp.mean(whole * whole, axis=1, keepdims=True) + EPSILON)
        out[:, cols] = (whole * scale * gate[:, cols]).astype(jnp.bfloat16)


def mix_kernel(*refs, ring, tp_count):
    blocks = refs[:ring]
    w_out, out_own, out_other, rows = refs[ring:]
    place = lax.axis_index("kv")
    own_rows = blocks[0].shape[0]
    half = out_own.shape[1]
    for shift in range(ring):
        source = lax.rem(place + ring - shift, ring)
        rows[pl.ds(pl.multiple_of(source * own_rows, own_rows), own_rows), :] = blocks[shift][...]
    tp_place = lax.axis_index("tp")
    for out, part in ((out_other, tp_count - 1 - tp_place), (out_own, tp_place)):
        at = pl.multiple_of(part * half, LANES)
        out[...] = jnp.dot(
            rows[...], w_out[:, pl.ds(at, half)], preferred_element_type=jnp.float32
        ).astype(jnp.bfloat16)


def finish_kernel(own, other, out):
    total = own[...].astype(jnp.float32) + other[...].astype(jnp.float32)
    props = out.shape[1]
    for seq in range(out.shape[0]):
        out[seq] = total[seq * props : (seq + 1) * props].astype(jnp.bfloat16)


def per_device(
    tokens,
    w_query,
    w_forget,
    w_input,
    w_gate,
    w_out,
    gain,
    head_gain,
    lower_bound,
    state,
    last_forget,
    last_values,
    accepted,
):
    group_seqs, props, feat = tokens.shape
    ring = lax.axis_size("kv")
    tp_count = lax.axis_size("tp")
    own_seqs = group_seqs // ring
    own_rows = own_seqs * props
    all_rows = group_seqs * props
    width = gain.shape[0]
    head_cols = w_query.shape[1]
    heads = head_cols // HEAD
    block = min(256, head_cols)

    def shifted(array, shift):
        return lax.ppermute(array, "kv", [(i, (i + shift) % ring) for i in range(ring)])

    order = sorted(range(1, ring), key=lambda shift: -min(shift, ring - shift))

    weight_spec = pl.BlockSpec((feat, block), lambda i: (0, i))
    whole = lambda *shape: pl.BlockSpec(shape, lambda i: (0,) * len(shape))
    sent_shape = (own_rows, 4 * head_cols + LANES)
    sent = pl.pallas_call(
        functools.partial(project_kernel, ring=ring, own_seqs=own_seqs, props=props),
        grid=(head_cols // block,),
        in_specs=[whole(*tokens.shape), whole(1, width)] + [weight_spec] * 4,
        out_specs=[whole(*sent_shape)] * ring,
        out_shape=[jax.ShapeDtypeStruct(sent_shape, jnp.bfloat16)] * ring,
        scratch_shapes=[
            pltpu.VMEM((all_rows, feat), jnp.float32),
            pltpu.VMEM((all_rows, feat), jnp.bfloat16),
        ],
        name="project",
    )(tokens, gain.reshape(1, width), w_query, w_forget, w_input, w_gate)

    received = [shifted(sent[shift], shift) for shift in order]

    taken = pl.pallas_call(
        taken_kernel,
        grid_spec=pltpu.PrefetchScalarGridSpec(
            num_scalar_prefetch=1,
            grid=(own_seqs,),
            in_specs=[
                pl.BlockSpec((1, heads, HEAD, HEAD), lambda i, _: (i, 0, 0, 0)),
                pl.BlockSpec((1, props, head_cols), lambda i, _: (i, 0, 0)),
                pl.BlockSpec((1, props, head_cols), lambda i, _: (i, 0, 0)),
            ],
            out_specs=pl.BlockSpec((1, heads, HEAD, HEAD), lambda i, _: (i, 0, 0, 0)),
        ),
        out_shape=jax.ShapeDtypeStruct(state.shape, jnp.float32),
        cost_estimate=pl.CostEstimate(
            flops=1 << 27, transcendentals=0, bytes_accessed=2 * 4 * state.size
        ),
        name="taken",
    )(accepted, state, last_forget, last_values)

    heads_out = pl.pallas_call(
        functools.partial(
            recur_kernel, ring=ring, own_seqs=own_seqs, props=props, width=width
        ),
        in_specs=[vmem_spec()] * (ring + 2) + [pl.BlockSpec(memory_space=pl.ANY)],
        out_specs=vmem_spec(),
        out_shape=jax.ShapeDtypeStruct((own_rows, head_cols), jnp.bfloat16),
        scratch_shapes=[pltpu.VMEM(state.shape, jnp.float32), pltpu.SemaphoreType.DMA],
        name="recur",
    )(
        sent[0],
        *received,
        lower_bound.reshape(1, -1),
        head_gain.reshape(1, -1),
        taken,
    )

    gathered = {shift: shifted(heads_out, shift) for shift in order}
    half = w_out.shape[1] // tp_count
    part_shape = jax.ShapeDtypeStruct((all_rows, half), jnp.bfloat16)
    own, other = pl.pallas_call(
        functools.partial(mix_kernel, ring=ring, tp_count=tp_count),
        in_specs=[vmem_spec()] * (ring + 1),
        out_specs=[vmem_spec()] * 2,
        out_shape=[part_shape] * 2,
        scratch_shapes=[pltpu.VMEM((all_rows, head_cols), jnp.bfloat16)],
        name="mix",
    )(heads_out, *[gathered[shift] for shift in range(1, ring)], w_out)
    swapped = lax.ppermute(other, "tp", [(i, tp_count - 1 - i) for i in range(tp_count)])
    mixed_out = pl.pallas_call(
        finish_kernel,
        in_specs=[vmem_spec()] * 2,
        out_specs=vmem_spec(),
        out_shape=jax.ShapeDtypeStruct((group_seqs, props, half), jnp.bfloat16),
        name="finish",
    )(own, swapped)
    return (mixed_out, taken)


def solution(mesh):
    in_specs = (
        P(("grp", "dp"), None, "kv"),
        P("kv", "tp"),
        P("kv", "tp"),
        P("kv", "tp"),
        P("kv", "tp"),
        P("tp", "kv"),
        P(),
        P(),
        P(),
        P(("grp", "dp", "kv"), "tp", None, None),
        P(("grp", "dp", "kv"), None, "tp"),
        P(("grp", "dp", "kv"), None, "tp"),
        P(("grp", "dp", "kv")),
    )
    out_specs = (P(("grp", "dp"), None, ("kv", "tp")), P(("grp", "dp", "kv"), "tp", None, None))
    return jax.shard_map(
        per_device, mesh=mesh, in_specs=in_specs, out_specs=out_specs, check_vma=False
    )
```

```python
import functools

import jax
import jax.numpy as jnp
from jax import lax
from jax.experimental import pallas as pl
from jax.experimental.pallas import tpu as pltpu
from jax.sharding import PartitionSpec as P

HEAD = 128
EPSILON = 1e-05
LANES = 128


def grant(mebibytes):
    return pltpu.CompilerParams(vmem_limit_bytes=mebibytes << 20)


def vmem_spec():
    return pl.BlockSpec(memory_space=pltpu.VMEM)


def project_kernel(tokens, gain, wq, wf, wi, wg, *rest, ring, own_seqs, props):
    outs, (rows_ref, scaled_ref) = rest[:ring], rest[ring:]
    step = pl.program_id(0)
    place = lax.axis_index("kv")
    feat = tokens.shape[2]
    own_rows = own_seqs * props
    head_cols = outs[0].shape[1] // 4 - LANES // 4
    block = wq.shape[1]

    @pl.when(step == 0)
    def _():
        for shift in range(ring):
            source = lax.rem(place + shift, ring) * own_seqs
            for seq in range(own_seqs):
                at = shift * own_rows + seq * props
                rows_ref[at : at + props, :] = tokens[source + seq].astype(jnp.float32)
        rows = rows_ref[...]
        local_gain = gain[:, pl.ds(pl.multiple_of(place * feat, LANES), feat)]
        scaled_ref[...] = (rows * local_gain).astype(jnp.bfloat16)
        total = jnp.sum(rows * rows, axis=1, keepdims=True)
        upper = total.astype(jnp.bfloat16).astype(jnp.float32)
        lane = lax.broadcasted_iota(jnp.int32, (rows.shape[0], LANES), 1)
        packed = jnp.where(lane == 0, upper, jnp.where(lane == 1, total - upper, 0.0))
        for shift in range(ring):
            outs[shift][:, 4 * head_cols :] = packed[
                shift * own_rows : (shift + 1) * own_rows
            ].astype(jnp.bfloat16)

    for index, weight in enumerate((wq, wf, wi, wg)):
        product = jnp.dot(scaled_ref[...], weight[...], preferred_element_type=jnp.float32)
        product = product.astype(jnp.bfloat16)
        at = pl.multiple_of(index * head_cols + step * block, LANES)
        for shift in range(ring):
            outs[shift][:, pl.ds(at, block)] = product[shift * own_rows : (shift + 1) * own_rows]


def taken_kernel(accepted, state, forget, values, taken, high, low):
    count = accepted[pl.program_id(0)]
    gates = forget[0]
    props, _ = gates.shape
    heads = state.shape[1]
    fresh = values[0].astype(jnp.float32)
    tail = jnp.ones_like(gates[:1])
    weights = [None] * props
    for at in reversed(range(props)):
        live = at < count
        gate = gates[at : at + 1]
        weights[at] = jnp.where(live, (1.0 - gate) * tail, 0.0)
        tail = jnp.where(live, gate * tail, tail)
    pad = jnp.zeros((8 - (props + 1) % 8, gates.shape[1]), jnp.float32)
    stacked = jnp.concatenate([tail] + weights + [pad], axis=0)
    for head in range(heads):
        cols = slice(head * HEAD, (head + 1) * HEAD)
        turned = stacked[:, cols].T
        total = turned[:, 0:1] * state[0, head]
        for at in range(props):
            total = total + turned[:, at + 1 : at + 2] * fresh[at : at + 1, cols]
        taken[0, head] = total
        rounded = total.astype(jnp.bfloat16)
        high[head] = rounded
        low[head] = (total - rounded.astype(jnp.float32)).astype(jnp.bfloat16)


def recur_kernel(*refs, ring, own_seqs, props, width):
    chunks = refs[:ring]
    floor, head_gain, high, low, out = refs[ring:]
    own_rows = own_seqs * props
    head_cols = out.shape[1]
    heads = head_cols // HEAD
    at_tp = pl.multiple_of(lax.axis_index("tp") * head_cols, LANES)
    floor_row = floor[:, pl.ds(at_tp, head_cols)]
    gain_row = head_gain[:, pl.ds(at_tp, head_cols)]

    def summed(start, size):
        total = chunks[0][:, start : start + size].astype(jnp.float32)
        for chunk in chunks[1:]:
            total = total + chunk[:, start : start + size].astype(jnp.float32)
        return total

    squares = jnp.sum(summed(4 * head_cols, LANES), axis=1, keepdims=True)
    row_scale = lax.rsqrt(squares / width + EPSILON)
    query_in = summed(0, head_cols) * row_scale
    queries = query_in * jax.nn.sigmoid(query_in) * HEAD ** (-0.5)
    forget = floor_row + (1.0 - floor_row) * jax.nn.sigmoid(
        summed(head_cols, head_cols) * row_scale
    )
    values = summed(2 * head_cols, head_cols) * row_scale
    gate_in = summed(3 * head_cols, head_cols) * row_scale
    gate = gate_in * jax.nn.sigmoid(gate_in) * gain_row
    keys = 1.0 - forget

    place = lax.broadcasted_iota(jnp.int32, (own_rows, 1), 0)
    token = lax.rem(place, props)
    seq = place // props
    decayed = queries
    entry = jnp.zeros_like(queries)
    recurrent = [jnp.zeros((own_rows, HEAD), jnp.float32) for _ in range(heads)]
    for back in range(props):
        old_keys = pltpu.roll(keys, back, 0) if back else keys
        old_values = pltpu.roll(values, back, 0) if back else values
        old_forget = pltpu.roll(forget, back, 0) if back else forget
        pair = decayed * old_keys
        for head in range(heads):
            cols = slice(head * HEAD, (head + 1) * HEAD)
            score = jnp.sum(pair[:, cols], axis=1, keepdims=True)
            score = jnp.where(token >= back, score, 0.0)
            recurrent[head] = recurrent[head] + score * old_values[:, cols]
        decayed = decayed * old_forget
        entry = jnp.where(token == back, decayed, entry)
    spread = []
    for head in range(heads):
        cols = slice(head * HEAD, (head + 1) * HEAD)
        spread.append(
            jnp.concatenate(
                [jnp.where(seq == one, entry[:, cols], 0.0) for one in range(own_seqs)], axis=1
            )
        )
    for head in range(heads):
        cols = slice(head * HEAD, (head + 1) * HEAD)
        start_high, start_low = high[head], low[head]
        left_high = spread[head].astype(jnp.bfloat16)
        left_low = (spread[head] - left_high.astype(jnp.float32)).astype(jnp.bfloat16)
        first = jnp.dot(
            jnp.concatenate([left_high, left_low], axis=0),
            start_high,
            preferred_element_type=jnp.float32,
        )
        second = jnp.dot(left_high, start_low, preferred_element_type=jnp.float32)
        whole = recurrent[head] + first[:own_rows] + first[own_rows:] + second
        scale = lax.rsqrt(jnp.mean(whole * whole, axis=1, keepdims=True) + EPSILON)
        out[:, cols] = (whole * scale * gate[:, cols]).astype(jnp.bfloat16)


def mix_kernel(*refs, ring, tp_count):
    blocks = refs[:ring]
    w_out, out_own, out_other, rows = refs[ring:]
    place = lax.axis_index("kv")
    own_rows = blocks[0].shape[0]
    half = out_own.shape[1]
    for shift in range(ring):
        source = lax.rem(place + ring - shift, ring)
        rows[pl.ds(pl.multiple_of(source * own_rows, own_rows), own_rows), :] = blocks[shift][...]
    tp_place = lax.axis_index("tp")
    for out, part in ((out_other, tp_count - 1 - tp_place), (out_own, tp_place)):
        at = pl.multiple_of(part * half, LANES)
        out[...] = jnp.dot(
            rows[...], w_out[:, pl.ds(at, half)], preferred_element_type=jnp.float32
        ).astype(jnp.bfloat16)


def finish_kernel(own, other, out):
    total = own[...].astype(jnp.float32) + other[...].astype(jnp.float32)
    props = out.shape[1]
    for seq in range(out.shape[0]):
        out[seq] = total[seq * props : (seq + 1) * props].astype(jnp.bfloat16)


def per_device(
    tokens,
    w_query,
    w_forget,
    w_input,
    w_gate,
    w_out,
    gain,
    head_gain,
    lower_bound,
    state,
    last_forget,
    last_values,
    accepted,
):
    group_seqs, props, feat = tokens.shape
    ring = lax.axis_size("kv")
    tp_count = lax.axis_size("tp")
    own_seqs = group_seqs // ring
    own_rows = own_seqs * props
    all_rows = group_seqs * props
    width = gain.shape[0]
    head_cols = w_query.shape[1]
    heads = head_cols // HEAD
    block = min(256, head_cols)

    def shifted(array, shift):
        return lax.ppermute(array, "kv", [(i, (i + shift) % ring) for i in range(ring)])

    order = sorted(range(1, ring), key=lambda shift: -min(shift, ring - shift))

    weight_spec = pl.BlockSpec((feat, block), lambda i: (0, i))
    whole = lambda *shape: pl.BlockSpec(shape, lambda i: (0,) * len(shape))
    sent_shape = (own_rows, 4 * head_cols + LANES)
    sent = pl.pallas_call(
        functools.partial(project_kernel, ring=ring, own_seqs=own_seqs, props=props),
        grid=(head_cols // block,),
        in_specs=[whole(*tokens.shape), whole(1, width)] + [weight_spec] * 4,
        out_specs=[whole(*sent_shape)] * ring,
        out_shape=[jax.ShapeDtypeStruct(sent_shape, jnp.bfloat16)] * ring,
        scratch_shapes=[
            pltpu.VMEM((all_rows, feat), jnp.float32),
            pltpu.VMEM((all_rows, feat), jnp.bfloat16),
        ],
        compiler_params=grant(52),
        name="project",
    )(tokens, gain.reshape(1, width), w_query, w_forget, w_input, w_gate)

    received = [shifted(sent[shift], shift) for shift in order]

    taken, high, low = pl.pallas_call(
        taken_kernel,
        grid_spec=pltpu.PrefetchScalarGridSpec(
            num_scalar_prefetch=1,
            grid=(own_seqs,),
            in_specs=[
                pl.BlockSpec((1, heads, HEAD, HEAD), lambda i, _: (i, 0, 0, 0)),
                pl.BlockSpec((1, props, head_cols), lambda i, _: (i, 0, 0)),
                pl.BlockSpec((1, props, head_cols), lambda i, _: (i, 0, 0)),
            ],
            out_specs=[
                pl.BlockSpec((1, heads, HEAD, HEAD), lambda i, _: (i, 0, 0, 0)),
                pl.BlockSpec((heads, HEAD, HEAD), lambda i, _: (0, i, 0)),
                pl.BlockSpec((heads, HEAD, HEAD), lambda i, _: (0, i, 0)),
            ],
        ),
        out_shape=[
            jax.ShapeDtypeStruct(state.shape, jnp.float32),
            jax.ShapeDtypeStruct((heads, own_seqs * HEAD, HEAD), jnp.bfloat16),
            jax.ShapeDtypeStruct((heads, own_seqs * HEAD, HEAD), jnp.bfloat16),
        ],
        cost_estimate=pl.CostEstimate(
            flops=1 << 27, transcendentals=0, bytes_accessed=2 * 4 * state.size
        ),
        compiler_params=grant(8),
        name="taken",
    )(accepted, state, last_forget, last_values)

    heads_out = pl.pallas_call(
        functools.partial(
            recur_kernel, ring=ring, own_seqs=own_seqs, props=props, width=width
        ),
        in_specs=[vmem_spec()] * (ring + 4),
        out_specs=vmem_spec(),
        out_shape=jax.ShapeDtypeStruct((own_rows, head_cols), jnp.bfloat16),
        compiler_params=grant(8),
        name="recur",
    )(
        sent[0],
        *received,
        lower_bound.reshape(1, -1),
        head_gain.reshape(1, -1),
        high,
        low,
    )

    gathered = {shift: shifted(heads_out, shift) for shift in order}
    half = w_out.shape[1] // tp_count
    part_shape = jax.ShapeDtypeStruct((all_rows, half), jnp.bfloat16)
    own, other = pl.pallas_call(
        functools.partial(mix_kernel, ring=ring, tp_count=tp_count),
        in_specs=[vmem_spec()] * (ring + 1),
        out_specs=[vmem_spec()] * 2,
        out_shape=[part_shape] * 2,
        scratch_shapes=[pltpu.VMEM((all_rows, head_cols), jnp.bfloat16)],
        compiler_params=grant(8),
        name="mix",
    )(heads_out, *[gathered[shift] for shift in range(1, ring)], w_out)
    swapped = lax.ppermute(other, "tp", [(i, tp_count - 1 - i) for i in range(tp_count)])
    mixed_out = pl.pallas_call(
        finish_kernel,
        in_specs=[vmem_spec()] * 2,
        out_specs=vmem_spec(),
        out_shape=jax.ShapeDtypeStruct((group_seqs, props, half), jnp.bfloat16),
        compiler_params=grant(4),
        name="finish",
    )(own, swapped)
    return (mixed_out, taken)


def solution(mesh):
    in_specs = (
        P(("grp", "dp"), None, "kv"),
        P("kv", "tp"),
        P("kv", "tp"),
        P("kv", "tp"),
        P("kv", "tp"),
        P("tp", "kv"),
        P(),
        P(),
        P(),
        P(("grp", "dp", "kv"), "tp", None, None),
        P(("grp", "dp", "kv"), None, "tp"),
        P(("grp", "dp", "kv"), None, "tp"),
        P(("grp", "dp", "kv")),
    )
    out_specs = (P(("grp", "dp"), None, ("kv", "tp")), P(("grp", "dp", "kv"), "tp", None, None))
    return jax.shard_map(
        per_device, mesh=mesh, in_specs=in_specs, out_specs=out_specs, check_vma=False
    )
```

```python
import functools

import jax
import jax.numpy as jnp
from jax import lax
from jax.experimental import pallas as pl
from jax.experimental.pallas import tpu as pltpu
from jax.sharding import PartitionSpec as P

HEAD = 128
EPSILON = 1e-05
LANES = 128


def grant(mebibytes):
    return pltpu.CompilerParams(vmem_limit_bytes=mebibytes << 20)


def vmem_spec():
    return pl.BlockSpec(memory_space=pltpu.VMEM)


def project_first_kernel(tokens, gain, *rest, ring, own_seqs, props, count):
    weights, outs = rest[:count], rest[count : count + ring]
    scaled_ref, rows_ref = rest[count + ring :]
    place = lax.axis_index("kv")
    feat = tokens.shape[2]
    own_rows = own_seqs * props
    head_cols = outs[0].shape[1] // count - LANES // count

    @pl.when(pl.program_id(0) == 0)
    def _():
        for shift in range(ring):
            source = lax.rem(place + shift, ring) * own_seqs
            for seq in range(own_seqs):
                at = shift * own_rows + seq * props
                rows_ref[at : at + props, :] = tokens[source + seq].astype(jnp.float32)
        rows = rows_ref[...]
        local_gain = gain[:, pl.ds(pl.multiple_of(place * feat, LANES), feat)]
        scaled_ref[...] = (rows * local_gain).astype(jnp.bfloat16)
        total = jnp.sum(rows * rows, axis=1, keepdims=True)
        upper = total.astype(jnp.bfloat16).astype(jnp.float32)
        lane = lax.broadcasted_iota(jnp.int32, (rows.shape[0], LANES), 1)
        packed = jnp.where(lane == 0, upper, jnp.where(lane == 1, total - upper, 0.0))
        for shift in range(ring):
            outs[shift][:, count * head_cols :] = packed[
                shift * own_rows : (shift + 1) * own_rows
            ].astype(jnp.bfloat16)

    multiply(scaled_ref, weights, outs, head_cols)


def project_next_kernel(scaled_ref, *rest, count):
    weights, outs = rest[:count], rest[count:]
    multiply(scaled_ref, weights, outs, outs[0].shape[1] // count)


def multiply(scaled_ref, weights, outs, head_cols):
    block = weights[0].shape[1]
    own_rows = outs[0].shape[0]
    for index, weight in enumerate(weights):
        product = jnp.dot(scaled_ref[...], weight[...], preferred_element_type=jnp.float32)
        product = product.astype(jnp.bfloat16)
        at = pl.multiple_of(index * head_cols + pl.program_id(0) * block, LANES)
        for shift, out in enumerate(outs):
            out[:, pl.ds(at, block)] = product[shift * own_rows : (shift + 1) * own_rows]


def taken_kernel(accepted, state, forget, values, taken, high, low):
    count = accepted[pl.program_id(0)]
    gates = forget[0]
    props, _ = gates.shape
    heads = state.shape[1]
    fresh = values[0].astype(jnp.float32)
    tail = jnp.ones_like(gates[:1])
    weights = [None] * props
    for at in reversed(range(props)):
        live = at < count
        gate = gates[at : at + 1]
        weights[at] = jnp.where(live, (1.0 - gate) * tail, 0.0)
        tail = jnp.where(live, gate * tail, tail)
    pad = jnp.zeros((8 - (props + 1) % 8, gates.shape[1]), jnp.float32)
    stacked = jnp.concatenate([tail] + weights + [pad], axis=0)
    for head in range(heads):
        cols = slice(head * HEAD, (head + 1) * HEAD)
        turned = stacked[:, cols].T
        total = turned[:, 0:1] * state[0, head]
        for at in range(props):
            total = total + turned[:, at + 1 : at + 2] * fresh[at : at + 1, cols]
        taken[0, head] = total
        rounded = total.astype(jnp.bfloat16)
        high[head] = rounded
        low[head] = (total - rounded.astype(jnp.float32)).astype(jnp.bfloat16)


def recur_kernel(*refs, ring, own_seqs, props, width):
    first, second = refs[:ring], refs[ring : 2 * ring]
    floor, head_gain, high, low, out = refs[2 * ring :]
    own_rows = own_seqs * props
    head_cols = out.shape[1]
    heads = head_cols // HEAD
    at_tp = pl.multiple_of(lax.axis_index("tp") * head_cols, LANES)
    floor_row = floor[:, pl.ds(at_tp, head_cols)]
    gain_row = head_gain[:, pl.ds(at_tp, head_cols)]

    def summed(chunks, start, size):
        total = chunks[0][:, start : start + size].astype(jnp.float32)
        for chunk in chunks[1:]:
            total = total + chunk[:, start : start + size].astype(jnp.float32)
        return total

    squares = jnp.sum(summed(first, 2 * head_cols, LANES), axis=1, keepdims=True)
    row_scale = lax.rsqrt(squares / width + EPSILON)
    query_in = summed(first, 0, head_cols) * row_scale
    queries = query_in * jax.nn.sigmoid(query_in) * HEAD ** (-0.5)
    forget = floor_row + (1.0 - floor_row) * jax.nn.sigmoid(
        summed(first, head_cols, head_cols) * row_scale
    )
    values = summed(second, 0, head_cols) * row_scale
    gate_in = summed(second, head_cols, head_cols) * row_scale
    gate = gate_in * jax.nn.sigmoid(gate_in) * gain_row
    keys = 1.0 - forget

    place = lax.broadcasted_iota(jnp.int32, (own_rows, 1), 0)
    token = lax.rem(place, props)
    seq = place // props
    decayed = queries
    entry = jnp.zeros_like(queries)
    recurrent = [jnp.zeros((own_rows, HEAD), jnp.float32) for _ in range(heads)]
    for back in range(props):
        old_keys = pltpu.roll(keys, back, 0) if back else keys
        old_values = pltpu.roll(values, back, 0) if back else values
        old_forget = pltpu.roll(forget, back, 0) if back else forget
        pair = decayed * old_keys
        for head in range(heads):
            cols = slice(head * HEAD, (head + 1) * HEAD)
            score = jnp.sum(pair[:, cols], axis=1, keepdims=True)
            score = jnp.where(token >= back, score, 0.0)
            recurrent[head] = recurrent[head] + score * old_values[:, cols]
        decayed = decayed * old_forget
        entry = jnp.where(token == back, decayed, entry)
    spread = []
    for head in range(heads):
        cols = slice(head * HEAD, (head + 1) * HEAD)
        spread.append(
            jnp.concatenate(
                [jnp.where(seq == one, entry[:, cols], 0.0) for one in range(own_seqs)], axis=1
            )
        )
    for head in range(heads):
        cols = slice(head * HEAD, (head + 1) * HEAD)
        start_high, start_low = high[head], low[head]
        left_high = spread[head].astype(jnp.bfloat16)
        left_low = (spread[head] - left_high.astype(jnp.float32)).astype(jnp.bfloat16)
        wide = jnp.dot(
            jnp.concatenate([left_high, left_low], axis=0),
            start_high,
            preferred_element_type=jnp.float32,
        )
        narrow = jnp.dot(left_high, start_low, preferred_element_type=jnp.float32)
        whole = recurrent[head] + wide[:own_rows] + wide[own_rows:] + narrow
        scale = lax.rsqrt(jnp.mean(whole * whole, axis=1, keepdims=True) + EPSILON)
        out[:, cols] = (whole * scale * gate[:, cols]).astype(jnp.bfloat16)


def mix_kernel(*refs, ring, tp_count):
    blocks = refs[:ring]
    w_out, out_own, out_other, rows = refs[ring:]
    place = lax.axis_index("kv")
    own_rows = blocks[0].shape[0]
    half = out_own.shape[1]
    for shift in range(ring):
        source = lax.rem(place + ring - shift, ring)
        rows[pl.ds(pl.multiple_of(source * own_rows, own_rows), own_rows), :] = blocks[shift][...]
    tp_place = lax.axis_index("tp")
    for out, part in ((out_other, tp_count - 1 - tp_place), (out_own, tp_place)):
        at = pl.multiple_of(part * half, LANES)
        out[...] = jnp.dot(
            rows[...], w_out[:, pl.ds(at, half)], preferred_element_type=jnp.float32
        ).astype(jnp.bfloat16)


def finish_kernel(own, other, out):
    total = own[...].astype(jnp.float32) + other[...].astype(jnp.float32)
    props = out.shape[1]
    for seq in range(out.shape[0]):
        out[seq] = total[seq * props : (seq + 1) * props].astype(jnp.bfloat16)


def per_device(
    tokens,
    w_query,
    w_forget,
    w_input,
    w_gate,
    w_out,
    gain,
    head_gain,
    lower_bound,
    state,
    last_forget,
    last_values,
    accepted,
):
    group_seqs, props, feat = tokens.shape
    ring = lax.axis_size("kv")
    tp_count = lax.axis_size("tp")
    own_seqs = group_seqs // ring
    own_rows = own_seqs * props
    all_rows = group_seqs * props
    width = gain.shape[0]
    head_cols = w_query.shape[1]
    heads = head_cols // HEAD
    block = min(256, head_cols)

    def shifted(array, shift):
        return lax.ppermute(array, "kv", [(i, (i + shift) % ring) for i in range(ring)])

    order = sorted(range(1, ring), key=lambda shift: -min(shift, ring - shift))

    weight_spec = pl.BlockSpec((feat, block), lambda i: (0, i))
    whole = lambda *shape: pl.BlockSpec(shape, lambda i: (0,) * len(shape))
    in_hbm = lambda array: pltpu.with_memory_space_constraint(array, pltpu.HBM)
    first_shape = (own_rows, 2 * head_cols + LANES)
    next_shape = (own_rows, 2 * head_cols)
    scaled_shape = (all_rows, feat)
    cost = pl.CostEstimate(
        flops=4 * all_rows * feat * head_cols,
        transcendentals=0,
        bytes_accessed=4 * feat * head_cols,
    )
    *sent_first, scaled = pl.pallas_call(
        functools.partial(
            project_first_kernel, ring=ring, own_seqs=own_seqs, props=props, count=2
        ),
        grid=(head_cols // block,),
        in_specs=[whole(*tokens.shape), whole(1, width)] + [weight_spec] * 2,
        out_specs=[whole(*first_shape)] * ring + [whole(*scaled_shape)],
        out_shape=[jax.ShapeDtypeStruct(first_shape, jnp.bfloat16)] * ring
        + [jax.ShapeDtypeStruct(scaled_shape, jnp.bfloat16)],
        scratch_shapes=[pltpu.VMEM(scaled_shape, jnp.float32)],
        compiler_params=grant(52),
        cost_estimate=cost,
        name="project_first",
    )(
        in_hbm(tokens),
        in_hbm(gain.reshape(1, width)),
        in_hbm(w_query),
        in_hbm(w_forget),
    )
    received_first = [shifted(sent_first[shift], shift) for shift in order]
    sent_next = pl.pallas_call(
        functools.partial(project_next_kernel, count=2),
        grid=(head_cols // block,),
        in_specs=[whole(*scaled_shape)] + [weight_spec] * 2,
        out_specs=[whole(*next_shape)] * ring,
        out_shape=[jax.ShapeDtypeStruct(next_shape, jnp.bfloat16)] * ring,
        compiler_params=grant(52),
        cost_estimate=cost,
        name="project_next",
    )(scaled, in_hbm(w_input), in_hbm(w_gate))
    received_next = [shifted(sent_next[shift], shift) for shift in order]

    taken, high, low = pl.pallas_call(
        taken_kernel,
        grid_spec=pltpu.PrefetchScalarGridSpec(
            num_scalar_prefetch=1,
            grid=(own_seqs,),
            in_specs=[
                pl.BlockSpec((1, heads, HEAD, HEAD), lambda i, _: (i, 0, 0, 0)),
                pl.BlockSpec((1, props, head_cols), lambda i, _: (i, 0, 0)),
                pl.BlockSpec((1, props, head_cols), lambda i, _: (i, 0, 0)),
            ],
            out_specs=[
                pl.BlockSpec((1, heads, HEAD, HEAD), lambda i, _: (i, 0, 0, 0)),
                pl.BlockSpec((heads, HEAD, HEAD), lambda i, _: (0, i, 0)),
                pl.BlockSpec((heads, HEAD, HEAD), lambda i, _: (0, i, 0)),
            ],
        ),
        out_shape=[
            jax.ShapeDtypeStruct(state.shape, jnp.float32),
            jax.ShapeDtypeStruct((heads, own_seqs * HEAD, HEAD), jnp.bfloat16),
            jax.ShapeDtypeStruct((heads, own_seqs * HEAD, HEAD), jnp.bfloat16),
        ],
        cost_estimate=pl.CostEstimate(
            flops=1 << 27, transcendentals=0, bytes_accessed=2 * 4 * state.size
        ),
        compiler_params=grant(8),
        name="taken",
    )(accepted, state, last_forget, last_values)

    heads_out = pl.pallas_call(
        functools.partial(
            recur_kernel, ring=ring, own_seqs=own_seqs, props=props, width=width
        ),
        in_specs=[vmem_spec()] * (2 * ring + 4),
        out_specs=vmem_spec(),
        out_shape=jax.ShapeDtypeStruct((own_rows, head_cols), jnp.bfloat16),
        compiler_params=grant(8),
        name="recur",
    )(
        sent_first[0],
        *received_first,
        sent_next[0],
        *received_next,
        lower_bound.reshape(1, -1),
        head_gain.reshape(1, -1),
        high,
        low,
    )

    gathered = {shift: shifted(heads_out, shift) for shift in order}
    half = w_out.shape[1] // tp_count
    part_shape = jax.ShapeDtypeStruct((all_rows, half), jnp.bfloat16)
    own, other = pl.pallas_call(
        functools.partial(mix_kernel, ring=ring, tp_count=tp_count),
        in_specs=[vmem_spec()] * (ring + 1),
        out_specs=[vmem_spec()] * 2,
        out_shape=[part_shape] * 2,
        scratch_shapes=[pltpu.VMEM((all_rows, head_cols), jnp.bfloat16)],
        compiler_params=grant(8),
        name="mix",
    )(heads_out, *[gathered[shift] for shift in range(1, ring)], w_out)
    swapped = lax.ppermute(other, "tp", [(i, tp_count - 1 - i) for i in range(tp_count)])
    mixed_out = pl.pallas_call(
        finish_kernel,
        in_specs=[vmem_spec()] * 2,
        out_specs=vmem_spec(),
        out_shape=jax.ShapeDtypeStruct((group_seqs, props, half), jnp.bfloat16),
        compiler_params=grant(4),
        name="finish",
    )(own, swapped)
    return (mixed_out, taken)


def solution(mesh):
    in_specs = (
        P(("grp", "dp"), None, "kv"),
        P("kv", "tp"),
        P("kv", "tp"),
        P("kv", "tp"),
        P("kv", "tp"),
        P("tp", "kv"),
        P(),
        P(),
        P(),
        P(("grp", "dp", "kv"), "tp", None, None),
        P(("grp", "dp", "kv"), None, "tp"),
        P(("grp", "dp", "kv"), None, "tp"),
        P(("grp", "dp", "kv")),
    )
    out_specs = (P(("grp", "dp"), None, ("kv", "tp")), P(("grp", "dp", "kv"), "tp", None, None))
    return jax.shard_map(
        per_device, mesh=mesh, in_specs=in_specs, out_specs=out_specs, check_vma=False
    )
```

```python
import functools

import jax
import jax.numpy as jnp
from jax import lax
from jax.experimental import pallas as pl
from jax.experimental.pallas import tpu as pltpu
from jax.sharding import PartitionSpec as P

HEAD = 128
EPSILON = 1e-05
LANES = 128


def grant(mebibytes):
    return pltpu.CompilerParams(vmem_limit_bytes=mebibytes << 20)


def vmem_spec():
    return pl.BlockSpec(memory_space=pltpu.VMEM)


def project_kernel(*refs, ring, own_seqs, props, block, depth):
    tokens_hbm, gain_hbm, *weights = refs[:6]
    outs = refs[6 : 6 + ring]
    tokens, gain, blocks, rows_ref, scaled_ref, token_sem, gain_sem, sems = refs[6 + ring :]
    place = lax.axis_index("kv")
    feat = tokens.shape[2]
    own_rows = own_seqs * props
    head_cols = weights[0].shape[1]
    at_gain = pl.multiple_of(place * feat, LANES)
    pieces = [
        (index * head_cols + start, weight, start)
        for index, weight in enumerate(weights)
        for start in range(0, head_cols, block)
    ]
    copies = [
        pltpu.make_async_copy(weight.at[:, pl.ds(start, block)], blocks.at[n], sems.at[n])
        for n, (_, weight, start) in enumerate(pieces)
    ]
    token_copy = pltpu.make_async_copy(tokens_hbm, tokens, token_sem)
    gain_copy = pltpu.make_async_copy(gain_hbm.at[:, pl.ds(at_gain, feat)], gain, gain_sem)
    token_copy.start()
    gain_copy.start()
    for copy in copies[:depth]:
        copy.start()
    token_copy.wait()
    gain_copy.wait()
    for shift in range(ring):
        source = lax.rem(place + shift, ring) * own_seqs
        for seq in range(own_seqs):
            at = shift * own_rows + seq * props
            rows_ref[at : at + props, :] = tokens[source + seq].astype(jnp.float32)
    rows = rows_ref[...]
    scaled_ref[...] = (rows * gain[...]).astype(jnp.bfloat16)
    total = jnp.sum(rows * rows, axis=1, keepdims=True)
    upper = total.astype(jnp.bfloat16).astype(jnp.float32)
    lane = lax.broadcasted_iota(jnp.int32, (rows.shape[0], LANES), 1)
    packed = jnp.where(lane == 0, upper, jnp.where(lane == 1, total - upper, 0.0))
    for shift in range(ring):
        outs[shift][:, 4 * head_cols :] = packed[
            shift * own_rows : (shift + 1) * own_rows
        ].astype(jnp.bfloat16)
    for n, (at, _, _) in enumerate(pieces):
        copies[n].wait()
        if n + depth < len(copies):
            copies[n + depth].start()
        product = jnp.dot(scaled_ref[...], blocks[n], preferred_element_type=jnp.float32)
        product = product.astype(jnp.bfloat16)
        for shift in range(ring):
            outs[shift][:, at : at + block] = product[shift * own_rows : (shift + 1) * own_rows]


def taken_kernel(accepted, state, forget, values, taken, high, low):
    count = accepted[pl.program_id(0)]
    gates = forget[0]
    props, _ = gates.shape
    heads = state.shape[1]
    fresh = values[0].astype(jnp.float32)
    tail = jnp.ones_like(gates[:1])
    weights = [None] * props
    for at in reversed(range(props)):
        live = at < count
        gate = gates[at : at + 1]
        weights[at] = jnp.where(live, (1.0 - gate) * tail, 0.0)
        tail = jnp.where(live, gate * tail, tail)
    pad = jnp.zeros((8 - (props + 1) % 8, gates.shape[1]), jnp.float32)
    stacked = jnp.concatenate([tail] + weights + [pad], axis=0)
    for head in range(heads):
        cols = slice(head * HEAD, (head + 1) * HEAD)
        turned = stacked[:, cols].T
        total = turned[:, 0:1] * state[0, head]
        for at in range(props):
            total = total + turned[:, at + 1 : at + 2] * fresh[at : at + 1, cols]
        taken[0, head] = total
        rounded = total.astype(jnp.bfloat16)
        high[head] = rounded
        low[head] = (total - rounded.astype(jnp.float32)).astype(jnp.bfloat16)


def recur_kernel(*refs, ring, own_seqs, props, width):
    chunks = refs[:ring]
    floor, head_gain, high, low, out = refs[ring:]
    own_rows = own_seqs * props
    head_cols = out.shape[1]
    heads = head_cols // HEAD
    at_tp = pl.multiple_of(lax.axis_index("tp") * head_cols, LANES)
    floor_row = floor[:, pl.ds(at_tp, head_cols)]
    gain_row = head_gain[:, pl.ds(at_tp, head_cols)]

    def summed(start, size):
        total = chunks[0][:, start : start + size].astype(jnp.float32)
        for chunk in chunks[1:]:
            total = total + chunk[:, start : start + size].astype(jnp.float32)
        return total

    squares = jnp.sum(summed(4 * head_cols, LANES), axis=1, keepdims=True)
    row_scale = lax.rsqrt(squares / width + EPSILON)
    query_in = summed(0, head_cols) * row_scale
    queries = query_in * jax.nn.sigmoid(query_in) * HEAD ** (-0.5)
    forget = floor_row + (1.0 - floor_row) * jax.nn.sigmoid(
        summed(head_cols, head_cols) * row_scale
    )
    values = summed(2 * head_cols, head_cols) * row_scale
    gate_in = summed(3 * head_cols, head_cols) * row_scale
    gate = gate_in * jax.nn.sigmoid(gate_in) * gain_row
    keys = 1.0 - forget

    place = lax.broadcasted_iota(jnp.int32, (own_rows, 1), 0)
    token = lax.rem(place, props)
    seq = place // props
    decayed = queries
    entry = jnp.zeros_like(queries)
    recurrent = [jnp.zeros((own_rows, HEAD), jnp.float32) for _ in range(heads)]
    for back in range(props):
        old_keys = pltpu.roll(keys, back, 0) if back else keys
        old_values = pltpu.roll(values, back, 0) if back else values
        old_forget = pltpu.roll(forget, back, 0) if back else forget
        pair = decayed * old_keys
        for head in range(heads):
            cols = slice(head * HEAD, (head + 1) * HEAD)
            score = jnp.sum(pair[:, cols], axis=1, keepdims=True)
            score = jnp.where(token >= back, score, 0.0)
            recurrent[head] = recurrent[head] + score * old_values[:, cols]
        decayed = decayed * old_forget
        entry = jnp.where(token == back, decayed, entry)
    spread = []
    for head in range(heads):
        cols = slice(head * HEAD, (head + 1) * HEAD)
        spread.append(
            jnp.concatenate(
                [jnp.where(seq == one, entry[:, cols], 0.0) for one in range(own_seqs)], axis=1
            )
        )
    for head in range(heads):
        cols = slice(head * HEAD, (head + 1) * HEAD)
        start_high, start_low = high[head], low[head]
        left_high = spread[head].astype(jnp.bfloat16)
        left_low = (spread[head] - left_high.astype(jnp.float32)).astype(jnp.bfloat16)
        first = jnp.dot(
            jnp.concatenate([left_high, left_low], axis=0),
            start_high,
            preferred_element_type=jnp.float32,
        )
        second = jnp.dot(left_high, start_low, preferred_element_type=jnp.float32)
        whole = recurrent[head] + first[:own_rows] + first[own_rows:] + second
        scale = lax.rsqrt(jnp.mean(whole * whole, axis=1, keepdims=True) + EPSILON)
        out[:, cols] = (whole * scale * gate[:, cols]).astype(jnp.bfloat16)


def mix_kernel(*refs, ring, tp_count):
    blocks = refs[:ring]
    w_out, out_own, out_other, rows = refs[ring:]
    place = lax.axis_index("kv")
    own_rows = blocks[0].shape[0]
    half = out_own.shape[1]
    for shift in range(ring):
        source = lax.rem(place + ring - shift, ring)
        rows[pl.ds(pl.multiple_of(source * own_rows, own_rows), own_rows), :] = blocks[shift][...]
    tp_place = lax.axis_index("tp")
    for out, part in ((out_other, tp_count - 1 - tp_place), (out_own, tp_place)):
        at = pl.multiple_of(part * half, LANES)
        out[...] = jnp.dot(
            rows[...], w_out[:, pl.ds(at, half)], preferred_element_type=jnp.float32
        ).astype(jnp.bfloat16)


def finish_kernel(own, other, out):
    total = own[...].astype(jnp.float32) + other[...].astype(jnp.float32)
    props = out.shape[1]
    for seq in range(out.shape[0]):
        out[seq] = total[seq * props : (seq + 1) * props].astype(jnp.bfloat16)


def per_device(
    tokens,
    w_query,
    w_forget,
    w_input,
    w_gate,
    w_out,
    gain,
    head_gain,
    lower_bound,
    state,
    last_forget,
    last_values,
    accepted,
):
    group_seqs, props, feat = tokens.shape
    ring = lax.axis_size("kv")
    tp_count = lax.axis_size("tp")
    own_seqs = group_seqs // ring
    own_rows = own_seqs * props
    all_rows = group_seqs * props
    width = gain.shape[0]
    head_cols = w_query.shape[1]
    heads = head_cols // HEAD
    block = min(256, head_cols)

    def shifted(array, shift):
        return lax.ppermute(array, "kv", [(i, (i + shift) % ring) for i in range(ring)])

    order = sorted(range(1, ring), key=lambda shift: -min(shift, ring - shift))

    in_hbm = lambda array: pltpu.with_memory_space_constraint(array, pltpu.HBM)
    sent_shape = (own_rows, 4 * head_cols + LANES)
    count = 4 * head_cols // block
    sent = pl.pallas_call(
        functools.partial(
            project_kernel, ring=ring, own_seqs=own_seqs, props=props, block=block, depth=6
        ),
        in_specs=[pl.BlockSpec(memory_space=pltpu.HBM)] * 6,
        out_specs=[vmem_spec()] * ring,
        out_shape=[jax.ShapeDtypeStruct(sent_shape, jnp.bfloat16)] * ring,
        scratch_shapes=[
            pltpu.VMEM(tokens.shape, jnp.bfloat16),
            pltpu.VMEM((1, feat), jnp.float32),
            pltpu.VMEM((count, feat, block), jnp.bfloat16),
            pltpu.VMEM((all_rows, feat), jnp.float32),
            pltpu.VMEM((all_rows, feat), jnp.bfloat16),
            pltpu.SemaphoreType.DMA,
            pltpu.SemaphoreType.DMA,
            pltpu.SemaphoreType.DMA((count,)),
        ],
        compiler_params=grant(16),
        name="project",
    )(
        in_hbm(tokens),
        in_hbm(gain.reshape(1, width)),
        in_hbm(w_query),
        in_hbm(w_forget),
        in_hbm(w_input),
        in_hbm(w_gate),
    )

    received = [shifted(sent[shift], shift) for shift in order]

    taken, high, low = pl.pallas_call(
        taken_kernel,
        grid_spec=pltpu.PrefetchScalarGridSpec(
            num_scalar_prefetch=1,
            grid=(own_seqs,),
            in_specs=[
                pl.BlockSpec((1, heads, HEAD, HEAD), lambda i, _: (i, 0, 0, 0)),
                pl.BlockSpec((1, props, head_cols), lambda i, _: (i, 0, 0)),
                pl.BlockSpec((1, props, head_cols), lambda i, _: (i, 0, 0)),
            ],
            out_specs=[
                pl.BlockSpec((1, heads, HEAD, HEAD), lambda i, _: (i, 0, 0, 0)),
                pl.BlockSpec((heads, HEAD, HEAD), lambda i, _: (0, i, 0)),
                pl.BlockSpec((heads, HEAD, HEAD), lambda i, _: (0, i, 0)),
            ],
        ),
        out_shape=[
            jax.ShapeDtypeStruct(state.shape, jnp.float32),
            jax.ShapeDtypeStruct((heads, own_seqs * HEAD, HEAD), jnp.bfloat16),
            jax.ShapeDtypeStruct((heads, own_seqs * HEAD, HEAD), jnp.bfloat16),
        ],
        cost_estimate=pl.CostEstimate(
            flops=1 << 27, transcendentals=0, bytes_accessed=2 * 4 * state.size
        ),
        compiler_params=grant(8),
        name="taken",
    )(accepted, state, last_forget, last_values)

    heads_out = pl.pallas_call(
        functools.partial(
            recur_kernel, ring=ring, own_seqs=own_seqs, props=props, width=width
        ),
        in_specs=[vmem_spec()] * (ring + 4),
        out_specs=vmem_spec(),
        out_shape=jax.ShapeDtypeStruct((own_rows, head_cols), jnp.bfloat16),
        compiler_params=grant(8),
        name="recur",
    )(
        sent[0],
        *received,
        lower_bound.reshape(1, -1),
        head_gain.reshape(1, -1),
        high,
        low,
    )

    gathered = {shift: shifted(heads_out, shift) for shift in order}
    half = w_out.shape[1] // tp_count
    part_shape = jax.ShapeDtypeStruct((all_rows, half), jnp.bfloat16)
    own, other = pl.pallas_call(
        functools.partial(mix_kernel, ring=ring, tp_count=tp_count),
        in_specs=[vmem_spec()] * (ring + 1),
        out_specs=[vmem_spec()] * 2,
        out_shape=[part_shape] * 2,
        scratch_shapes=[pltpu.VMEM((all_rows, head_cols), jnp.bfloat16)],
        compiler_params=grant(8),
        name="mix",
    )(heads_out, *[gathered[shift] for shift in range(1, ring)], w_out)
    swapped = lax.ppermute(other, "tp", [(i, tp_count - 1 - i) for i in range(tp_count)])
    mixed_out = pl.pallas_call(
        finish_kernel,
        in_specs=[vmem_spec()] * 2,
        out_specs=vmem_spec(),
        out_shape=jax.ShapeDtypeStruct((group_seqs, props, half), jnp.bfloat16),
        compiler_params=grant(4),
        name="finish",
    )(own, swapped)
    return (mixed_out, taken)


def solution(mesh):
    in_specs = (
        P(("grp", "dp"), None, "kv"),
        P("kv", "tp"),
        P("kv", "tp"),
        P("kv", "tp"),
        P("kv", "tp"),
        P("tp", "kv"),
        P(),
        P(),
        P(),
        P(("grp", "dp", "kv"), "tp", None, None),
        P(("grp", "dp", "kv"), None, "tp"),
        P(("grp", "dp", "kv"), None, "tp"),
        P(("grp", "dp", "kv")),
    )
    out_specs = (P(("grp", "dp"), None, ("kv", "tp")), P(("grp", "dp", "kv"), "tp", None, None))
    return jax.shard_map(
        per_device, mesh=mesh, in_specs=in_specs, out_specs=out_specs, check_vma=False
    )
```

```python
import functools

import jax
import jax.numpy as jnp
from jax import lax
from jax.experimental import pallas as pl
from jax.experimental.pallas import tpu as pltpu
from jax.sharding import PartitionSpec as P

HEAD = 128
EPSILON = 1e-05
LANES = 128


def grant(mebibytes):
    return pltpu.CompilerParams(vmem_limit_bytes=mebibytes << 20)


def vmem_spec():
    return pl.BlockSpec(memory_space=pltpu.VMEM)


def project_kernel(*refs, ring, own_seqs, props, block, depth):
    tokens_hbm, gain_hbm, *weights = refs[:6]
    outs = refs[6 : 6 + ring]
    tokens, gain, blocks, rows_ref, scaled_ref, token_sem, gain_sem, sems = refs[6 + ring :]
    place = lax.axis_index("kv")
    feat = tokens.shape[2]
    own_rows = own_seqs * props
    head_cols = weights[0].shape[1]
    at_gain = pl.multiple_of(place * feat, LANES)
    pieces = [
        (index * head_cols + start, weight, start)
        for index, weight in enumerate(weights)
        for start in range(0, head_cols, block)
    ]
    copies = [
        pltpu.make_async_copy(weight.at[:, pl.ds(start, block)], blocks.at[n], sems.at[n])
        for n, (_, weight, start) in enumerate(pieces)
    ]
    token_copy = pltpu.make_async_copy(tokens_hbm, tokens, token_sem)
    gain_copy = pltpu.make_async_copy(gain_hbm.at[:, pl.ds(at_gain, feat)], gain, gain_sem)
    token_copy.start()
    gain_copy.start()
    for copy in copies[:depth]:
        copy.start()
    token_copy.wait()
    gain_copy.wait()
    for shift in range(ring):
        source = lax.rem(place + shift, ring) * own_seqs
        for seq in range(own_seqs):
            at = shift * own_rows + seq * props
            rows_ref[at : at + props, :] = tokens[source + seq].astype(jnp.float32)
    rows = rows_ref[...]
    scaled_ref[...] = (rows * gain[...]).astype(jnp.bfloat16)
    total = jnp.sum(rows * rows, axis=1, keepdims=True)
    upper = total.astype(jnp.bfloat16).astype(jnp.float32)
    lane = lax.broadcasted_iota(jnp.int32, (rows.shape[0], LANES), 1)
    packed = jnp.where(lane == 0, upper, jnp.where(lane == 1, total - upper, 0.0))
    for shift in range(ring):
        outs[shift][:, 4 * head_cols :] = packed[
            shift * own_rows : (shift + 1) * own_rows
        ].astype(jnp.bfloat16)
    for n, (at, _, _) in enumerate(pieces):
        copies[n].wait()
        if n + depth < len(copies):
            copies[n + depth].start()
        product = jnp.dot(scaled_ref[...], blocks[n], preferred_element_type=jnp.float32)
        product = product.astype(jnp.bfloat16)
        for shift in range(ring):
            outs[shift][:, at : at + block] = product[shift * own_rows : (shift + 1) * own_rows]


def taken_kernel(accepted, state, forget, values, taken, high, low):
    count = accepted[pl.program_id(0)]
    gates = forget[0]
    props, _ = gates.shape
    heads = state.shape[1]
    fresh = values[0].astype(jnp.float32)
    tail = jnp.ones_like(gates[:1])
    weights = [None] * props
    for at in reversed(range(props)):
        live = at < count
        gate = gates[at : at + 1]
        weights[at] = jnp.where(live, (1.0 - gate) * tail, 0.0)
        tail = jnp.where(live, gate * tail, tail)
    pad = jnp.zeros((8 - (props + 1) % 8, gates.shape[1]), jnp.float32)
    stacked = jnp.concatenate([tail] + weights + [pad], axis=0)
    for head in range(heads):
        cols = slice(head * HEAD, (head + 1) * HEAD)
        turned = stacked[:, cols].T
        total = turned[:, 0:1] * state[0, head]
        for at in range(props):
            total = total + turned[:, at + 1 : at + 2] * fresh[at : at + 1, cols]
        taken[0, head] = total
        rounded = total.astype(jnp.bfloat16)
        high[head] = rounded
        low[head] = (total - rounded.astype(jnp.float32)).astype(jnp.bfloat16)


def recur_kernel(*refs, ring, own_seqs, props, width):
    chunks = refs[:ring]
    floor, head_gain, high, low, out = refs[ring:]
    own_rows = own_seqs * props
    head_cols = out.shape[1]
    heads = head_cols // HEAD
    at_tp = pl.multiple_of(lax.axis_index("tp") * head_cols, LANES)
    floor_row = floor[:, pl.ds(at_tp, head_cols)]
    gain_row = head_gain[:, pl.ds(at_tp, head_cols)]

    def summed(start, size):
        total = chunks[0][:, start : start + size].astype(jnp.float32)
        for chunk in chunks[1:]:
            total = total + chunk[:, start : start + size].astype(jnp.float32)
        return total

    squares = jnp.sum(summed(4 * head_cols, LANES), axis=1, keepdims=True)
    row_scale = lax.rsqrt(squares / width + EPSILON)
    query_in = summed(0, head_cols) * row_scale
    queries = query_in * jax.nn.sigmoid(query_in) * HEAD ** (-0.5)
    forget = floor_row + (1.0 - floor_row) * jax.nn.sigmoid(
        summed(head_cols, head_cols) * row_scale
    )
    values = summed(2 * head_cols, head_cols) * row_scale
    gate_in = summed(3 * head_cols, head_cols) * row_scale
    gate = gate_in * jax.nn.sigmoid(gate_in) * gain_row
    keys = 1.0 - forget

    place = lax.broadcasted_iota(jnp.int32, (own_rows, 1), 0)
    token = lax.rem(place, props)
    seq = place // props
    decayed = queries
    entry = jnp.zeros_like(queries)
    recurrent = [jnp.zeros((own_rows, HEAD), jnp.float32) for _ in range(heads)]
    for back in range(props):
        old_keys = pltpu.roll(keys, back, 0) if back else keys
        old_values = pltpu.roll(values, back, 0) if back else values
        old_forget = pltpu.roll(forget, back, 0) if back else forget
        pair = decayed * old_keys
        for head in range(heads):
            cols = slice(head * HEAD, (head + 1) * HEAD)
            score = jnp.sum(pair[:, cols], axis=1, keepdims=True)
            score = jnp.where(token >= back, score, 0.0)
            recurrent[head] = recurrent[head] + score * old_values[:, cols]
        decayed = decayed * old_forget
        entry = jnp.where(token == back, decayed, entry)
    spread = []
    for head in range(heads):
        cols = slice(head * HEAD, (head + 1) * HEAD)
        spread.append(
            jnp.concatenate(
                [jnp.where(seq == one, entry[:, cols], 0.0) for one in range(own_seqs)], axis=1
            )
        )
    for head in range(heads):
        cols = slice(head * HEAD, (head + 1) * HEAD)
        start_high, start_low = high[head], low[head]
        left_high = spread[head].astype(jnp.bfloat16)
        left_low = (spread[head] - left_high.astype(jnp.float32)).astype(jnp.bfloat16)
        first = jnp.dot(
            jnp.concatenate([left_high, left_low], axis=0),
            start_high,
            preferred_element_type=jnp.float32,
        )
        second = jnp.dot(left_high, start_low, preferred_element_type=jnp.float32)
        whole = recurrent[head] + first[:own_rows] + first[own_rows:] + second
        scale = lax.rsqrt(jnp.mean(whole * whole, axis=1, keepdims=True) + EPSILON)
        out[:, cols] = (whole * scale * gate[:, cols]).astype(jnp.bfloat16)


def mix_kernel(*refs, ring, tp_count):
    blocks = refs[:ring]
    w_out, out_own, out_other, rows = refs[ring:]
    place = lax.axis_index("kv")
    own_rows = blocks[0].shape[0]
    half = out_own.shape[1]
    for shift in range(ring):
        source = lax.rem(place + ring - shift, ring)
        rows[pl.ds(pl.multiple_of(source * own_rows, own_rows), own_rows), :] = blocks[shift][...]
    tp_place = lax.axis_index("tp")
    for out, part in ((out_other, tp_count - 1 - tp_place), (out_own, tp_place)):
        at = pl.multiple_of(part * half, LANES)
        out[...] = jnp.dot(
            rows[...], w_out[:, pl.ds(at, half)], preferred_element_type=jnp.float32
        ).astype(jnp.bfloat16)


def finish_kernel(own, other, out):
    total = own[...].astype(jnp.float32) + other[...].astype(jnp.float32)
    props = out.shape[1]
    for seq in range(out.shape[0]):
        out[seq] = total[seq * props : (seq + 1) * props].astype(jnp.bfloat16)


def per_device(
    tokens,
    w_query,
    w_forget,
    w_input,
    w_gate,
    w_out,
    gain,
    head_gain,
    lower_bound,
    state,
    last_forget,
    last_values,
    accepted,
):
    group_seqs, props, feat = tokens.shape
    ring = lax.axis_size("kv")
    tp_count = lax.axis_size("tp")
    own_seqs = group_seqs // ring
    own_rows = own_seqs * props
    all_rows = group_seqs * props
    width = gain.shape[0]
    head_cols = w_query.shape[1]
    heads = head_cols // HEAD
    block = min(512, head_cols)

    def shifted(array, shift):
        return lax.ppermute(array, "kv", [(i, (i + shift) % ring) for i in range(ring)])

    order = sorted(range(1, ring), key=lambda shift: -min(shift, ring - shift))

    in_hbm = lambda array: pltpu.with_memory_space_constraint(array, pltpu.HBM)
    sent_shape = (own_rows, 4 * head_cols + LANES)
    count = 4 * head_cols // block
    sent = pl.pallas_call(
        functools.partial(
            project_kernel, ring=ring, own_seqs=own_seqs, props=props, block=block, depth=4
        ),
        in_specs=[pl.BlockSpec(memory_space=pltpu.HBM)] * 6,
        out_specs=[vmem_spec()] * ring,
        out_shape=[jax.ShapeDtypeStruct(sent_shape, jnp.bfloat16)] * ring,
        scratch_shapes=[
            pltpu.VMEM(tokens.shape, jnp.bfloat16),
            pltpu.VMEM((1, feat), jnp.float32),
            pltpu.VMEM((count, feat, block), jnp.bfloat16),
            pltpu.VMEM((all_rows, feat), jnp.float32),
            pltpu.VMEM((all_rows, feat), jnp.bfloat16),
            pltpu.SemaphoreType.DMA,
            pltpu.SemaphoreType.DMA,
            pltpu.SemaphoreType.DMA((count,)),
        ],
        compiler_params=grant(16),
        name="project",
    )(
        in_hbm(tokens),
        in_hbm(gain.reshape(1, width)),
        in_hbm(w_query),
        in_hbm(w_forget),
        in_hbm(w_input),
        in_hbm(w_gate),
    )

    received = [shifted(sent[shift], shift) for shift in order]

    taken, high, low = pl.pallas_call(
        taken_kernel,
        grid_spec=pltpu.PrefetchScalarGridSpec(
            num_scalar_prefetch=1,
            grid=(own_seqs,),
            in_specs=[
                pl.BlockSpec((1, heads, HEAD, HEAD), lambda i, _: (i, 0, 0, 0)),
                pl.BlockSpec((1, props, head_cols), lambda i, _: (i, 0, 0)),
                pl.BlockSpec((1, props, head_cols), lambda i, _: (i, 0, 0)),
            ],
            out_specs=[
                pl.BlockSpec((1, heads, HEAD, HEAD), lambda i, _: (i, 0, 0, 0)),
                pl.BlockSpec((heads, HEAD, HEAD), lambda i, _: (0, i, 0)),
                pl.BlockSpec((heads, HEAD, HEAD), lambda i, _: (0, i, 0)),
            ],
        ),
        out_shape=[
            jax.ShapeDtypeStruct(state.shape, jnp.float32),
            jax.ShapeDtypeStruct((heads, own_seqs * HEAD, HEAD), jnp.bfloat16),
            jax.ShapeDtypeStruct((heads, own_seqs * HEAD, HEAD), jnp.bfloat16),
        ],
        cost_estimate=pl.CostEstimate(
            flops=1 << 27, transcendentals=0, bytes_accessed=2 * 4 * state.size
        ),
        compiler_params=grant(8),
        name="taken",
    )(accepted, state, last_forget, last_values)

    heads_out = pl.pallas_call(
        functools.partial(
            recur_kernel, ring=ring, own_seqs=own_seqs, props=props, width=width
        ),
        in_specs=[vmem_spec()] * (ring + 4),
        out_specs=vmem_spec(),
        out_shape=jax.ShapeDtypeStruct((own_rows, head_cols), jnp.bfloat16),
        compiler_params=grant(8),
        name="recur",
    )(
        sent[0],
        *received,
        lower_bound.reshape(1, -1),
        head_gain.reshape(1, -1),
        high,
        low,
    )

    gathered = {shift: shifted(heads_out, shift) for shift in order}
    half = w_out.shape[1] // tp_count
    part_shape = jax.ShapeDtypeStruct((all_rows, half), jnp.bfloat16)
    own, other = pl.pallas_call(
        functools.partial(mix_kernel, ring=ring, tp_count=tp_count),
        in_specs=[vmem_spec()] * (ring + 1),
        out_specs=[vmem_spec()] * 2,
        out_shape=[part_shape] * 2,
        scratch_shapes=[pltpu.VMEM((all_rows, head_cols), jnp.bfloat16)],
        compiler_params=grant(8),
        name="mix",
    )(heads_out, *[gathered[shift] for shift in range(1, ring)], w_out)
    swapped = lax.ppermute(other, "tp", [(i, tp_count - 1 - i) for i in range(tp_count)])
    mixed_out = pl.pallas_call(
        finish_kernel,
        in_specs=[vmem_spec()] * 2,
        out_specs=vmem_spec(),
        out_shape=jax.ShapeDtypeStruct((group_seqs, props, half), jnp.bfloat16),
        compiler_params=grant(4),
        name="finish",
    )(own, swapped)
    return (mixed_out, taken)


def solution(mesh):
    in_specs = (
        P(("grp", "dp"), None, "kv"),
        P("kv", "tp"),
        P("kv", "tp"),
        P("kv", "tp"),
        P("kv", "tp"),
        P("tp", "kv"),
        P(),
        P(),
        P(),
        P(("grp", "dp", "kv"), "tp", None, None),
        P(("grp", "dp", "kv"), None, "tp"),
        P(("grp", "dp", "kv"), None, "tp"),
        P(("grp", "dp", "kv")),
    )
    out_specs = (P(("grp", "dp"), None, ("kv", "tp")), P(("grp", "dp", "kv"), "tp", None, None))
    return jax.shard_map(
        per_device, mesh=mesh, in_specs=in_specs, out_specs=out_specs, check_vma=False
    )
```
